32 devices in a mesh: grp: 2 (over y), fs: 4 (over z), tp: 4 (over x, core).
Axes of the slice: x: 2, y: 2, z: 4, core: 2. Of those that a mesh axis runs over, the one named last changes fastest.
Arguments:
- tokens: bfloat16 [4096, 2048], P(('grp', 'tp')), parts along dimension 0, may hold values from -6 to 6
- gate_weight: float32 [2, 2048, 5632], P(None, 'fs', 'tp'), may hold values from -0.125 to 0.125
- up_weight: float32 [2, 2048, 5632], P(None, 'fs', 'tp'), may hold values from -0.125 to 0.125
- down_weight: float32 [2, 2048, 5632], P(None, 'fs', 'tp'), may hold values from -0.078125 to 0.078125
- in_gain: float32 [2, 2048], P(None, 'fs'), may hold values from 0.1 to 1.9
- out_gain: float32 [2, 2048], replicated, may hold values from 0.1 to 1.9
Outputs:
- sampler_gate: bfloat16 [4, 2048, 5632], P('grp', None, 'fs'), parts along dimension 0
- sampler_up: bfloat16 [4, 2048, 5632], P('grp', None, 'fs'), parts along dimension 0
- sampler_down: bfloat16 [4, 2048, 5632], P('grp', None, 'fs'), parts along dimension 0
- result: bfloat16 [4096, 2048], P(('grp', 'tp', 'fs')), parts along dimension 0
The draws below stay inside these ranges and needn't reach their ends.
There are 2 independent parts, one for each index of `grp`. The reference program is written for one: setup_inputs(seed, part) draws one part's arguments, and reference() takes and returns one part's arrays. A program takes and returns all parts, laid end to end along the dimension named above; an argument that names none is the same for every part. Nothing has to cross between parts.
All inputs are finite; a program needn't handle non-finite values.
Results may differ from the reference program's by a relative error of at most 0.0073.
Values may be sent and summed in bfloat16 or wider, within the bound.
A program may use at most 192 MiB of HBM per device.

```python
import jax
import jax.numpy as jnp
from jax import lax

D = 2048
FF = 5632
TOKENS = 2048
HB = 352
N_FS = 4
N_TP = 4


def levels(stream_key, extent, shards, least, largest):
    loudness, own = 1.0, jax.random.fold_in(stream_key, 6)
    for position, shards_of in shards:
        draws = jnp.exp(jax.random.uniform(jax.random.fold_in(own, position), (shards_of,), jnp.float32, least / len(shards), largest / len(shards)))
        loudness = loudness * jnp.repeat(draws, extent[position] // shards_of).reshape([-1 if axis == position else 1 for axis in range(len(extent))])
    return loudness


def centred(stream_key, dims, width, bound, pieces=(), kind=jnp.bfloat16):
    entries = width * jax.random.normal(stream_key, dims, jnp.float32)
    if pieces:
        entries = entries * levels(stream_key, dims, pieces, -0.22, 0.18)
    return jnp.clip(entries, -bound, bound).astype(kind)


def setup_inputs(seed: int = 0, part: int = 0) -> dict:
    arg_keys = jax.random.split(jax.random.key(seed), 7)
    own_keys = jax.random.split(jax.random.fold_in(arg_keys[6], part), 7)
    return {
        "tokens": centred(own_keys[0], (TOKENS, D), 1.0, 6.0, ((0, 4),)),
        "gate_weight": centred(arg_keys[1], (2, D, FF), D ** -0.5, 0.125, ((1, 4), (2, 4)), jnp.float32),
        "up_weight": centred(arg_keys[2], (2, D, FF), D ** -0.5, 0.125, ((1, 4), (2, 4)), jnp.float32),
        "down_weight": centred(arg_keys[3], (2, D, FF), FF ** -0.5, 0.078125, ((1, 4), (2, 4)), jnp.float32),
        "in_gain": jnp.clip(1.0 + 0.18 * jax.random.normal(arg_keys[4], (2, D), jnp.float32), 0.1, 1.9),
        "out_gain": jnp.clip(1.0 + 0.18 * jax.random.normal(arg_keys[5], (2, D), jnp.float32), 0.1, 1.9),
    }


EPS = 1e-06

def normalize(rows):
    return rows * lax.rsqrt(lax.optimization_barrier(jnp.mean(rows * rows, axis=-1, keepdims=True)) + EPS)

def reorder(matrix):
    return matrix.reshape(D, N_TP, N_FS, HB).transpose(0, 2, 1, 3).reshape(D, FF)

def reference(tokens, gate_weight, up_weight, down_weight, in_gain, out_gain):
    gates = []
    ups = []
    downs = []
    state = tokens.astype(jnp.float32)
    rounded = tokens
    for section_idx in range(2):
        gate_matrix = (in_gain[section_idx][:, None] * gate_weight[section_idx]).astype(jnp.bfloat16)
        up_matrix = (in_gain[section_idx][:, None] * up_weight[section_idx]).astype(jnp.bfloat16)
        down_matrix = down_weight[section_idx].astype(jnp.bfloat16)
        gates.append(reorder(gate_matrix))
        ups.append(reorder(up_matrix))
        downs.append(reorder(down_matrix))
        normed = normalize(state).astype(jnp.bfloat16)
        gate_act = jnp.dot(normed, gate_matrix, preferred_element_type=jnp.float32)
        up_act = jnp.dot(normed, up_matrix, preferred_element_type=jnp.float32)
        hidden = (jax.nn.silu(gate_act) * up_act).astype(jnp.bfloat16)
        mixed = lax.dot_general(hidden, down_matrix, (((1,), (1,)), ((), ())), preferred_element_type=jnp.float32)
        rounded = lax.optimization_barrier((state + 0.5 * out_gain[section_idx] * normalize(mixed)).astype(jnp.bfloat16))
        state = rounded.astype(jnp.float32)
    return (jnp.stack(gates), jnp.stack(ups), jnp.stack(downs), rounded)
```

```python
import functools

import jax
import jax.numpy as jnp
from jax import lax
from jax.experimental import pallas as pl
from jax.experimental.pallas import tpu as pltpu
from jax.sharding import PartitionSpec as P

EPS = 1e-06


def normalize(rows):
    return rows * lax.rsqrt(jnp.mean(rows * rows, axis=-1, keepdims=True) + EPS)


def body_plain(tokens, gate_weight, up_weight, down_weight, in_gain, out_gain):
    groups = lax.axis_size("fs")
    rows_all = tokens.shape[0]
    rows_mine = rows_all // groups
    model_width = tokens.shape[1]
    local_rows = gate_weight.shape[1]
    block_width = gate_weight.shape[2] // groups
    residual = lax.dynamic_slice_in_dim(
        tokens, lax.axis_index("fs") * rows_mine, rows_mine, 0
    ).astype(jnp.float32)
    normed = normalize(tokens.astype(jnp.float32)).astype(jnp.bfloat16)
    gates = []
    ups = []
    downs = []
    rounded_state = tokens
    contract_last = (((1,), (1,)), ((), ()))
    for section_idx in range(2):
        scale = in_gain[section_idx][:, None]
        gate_rounded = (scale * gate_weight[section_idx]).astype(jnp.bfloat16)
        up_rounded = (scale * up_weight[section_idx]).astype(jnp.bfloat16)
        down_rounded = down_weight[section_idx].astype(jnp.bfloat16)
        flipped = [
            w.T.reshape(groups, block_width, local_rows)
            for w in (gate_rounded, up_rounded, down_rounded)
        ]
        arrived = (
            lax.all_to_all(flipped[0], "fs", split_axis=0, concat_axis=2, tiled=True),
            lax.all_to_all(flipped[1], "fs", split_axis=0, concat_axis=2, tiled=True),
            lax.all_to_all(flipped[2], "fs", split_axis=0, concat_axis=2, tiled=True),
        )
        thin_rows = [w.reshape(block_width, model_width) for w in arrived]
        sampler_mats = (
            lax.all_gather(thin_rows[0], "tp", axis=0, tiled=True),
            lax.all_gather(thin_rows[1], "tp", axis=0, tiled=True),
            lax.all_gather(thin_rows[2], "tp", axis=0, tiled=True),
        )
        gate_flip, up_flip, down_flip = (sampler_mats[0], sampler_mats[1], sampler_mats[2])
        gates.append(gate_flip.T)
        ups.append(up_flip.T)
        downs.append(down_flip.T)

        def hidden_of(row_block):
            gate_act = lax.dot_general(
                row_block, gate_flip, contract_last, preferred_element_type=jnp.float32
            )
            up_act = lax.dot_general(
                row_block, up_flip, contract_last, preferred_element_type=jnp.float32
            )
            return (jax.nn.silu(gate_act) * up_act).astype(jnp.bfloat16)

        if section_idx == 0:
            hidden = hidden_of(normed)
        else:
            hidden = hidden_of(lax.all_gather(normed, "fs", axis=0, tiled=True))
        mixed = lax.psum_scatter(
            jnp.dot(hidden, down_flip, preferred_element_type=jnp.float32),
            "fs",
            scatter_dimension=0,
            tiled=True,
        )
        rounded_state = (residual + 0.5 * out_gain[section_idx] * normalize(mixed)).astype(
            jnp.bfloat16
        )
        if section_idx == 0:
            residual = rounded_state.astype(jnp.float32)
            normed = normalize(residual).astype(jnp.bfloat16)
    return (jnp.stack(gates), jnp.stack(ups), jnp.stack(downs), rounded_state)


def prep_kernel(blocks, width, part, scaled, where, *refs):
    if scaled:
        gain, weight, *outs, flip = refs
        rows = weight[0] * gain[0]
    else:
        weight, *outs, flip = refs
        rows = weight[0]
    flip[...] = rows.astype(jnp.bfloat16).T
    for shift in range(blocks):
        target = lax.rem(where[0] + shift, blocks)
        start = pl.multiple_of(target * width + where[1] * part, 16)
        outs[shift][...] = flip[pl.ds(start, part), :]


def prepare(where, weight, gain, layer, blocks, halves):
    _, rows, cols = weight.shape
    width = cols // blocks
    part = width // halves
    step = 256 if rows % 256 == 0 else rows
    in_specs = [pl.BlockSpec((1, step, cols), lambda r, where: (layer, r, 0))]
    args = [weight]
    if gain is not None:
        in_specs.insert(0, pl.BlockSpec((1, step, 1), lambda r, where: (layer, r, 0)))
        args.insert(0, gain)
    return pl.pallas_call(
        functools.partial(prep_kernel, blocks, width, part, gain is not None),
        grid_spec=pltpu.PrefetchScalarGridSpec(
            num_scalar_prefetch=1,
            grid=(rows // step,),
            in_specs=in_specs,
            out_specs=[pl.BlockSpec((part, step), lambda r, where: (0, r))] * blocks,
            scratch_shapes=[pltpu.VMEM((cols, step), jnp.bfloat16)],
        ),
        out_shape=[jax.ShapeDtypeStruct((part, rows), jnp.bfloat16)] * blocks,
        cost_estimate=pl.CostEstimate(
            flops=rows * cols, bytes_accessed=rows * cols * 5, transcendentals=0
        ),
    )(where, *args)


def join_kernel(blocks, where, *refs):
    *pieces, out = refs
    wide = pieces[0].shape[1]
    for shift in range(blocks):
        source = lax.rem(where[0] + blocks - shift, blocks)
        out[:, pl.ds(pl.multiple_of(source * wide, 128), wide)] = pieces[shift][...]


def join(where, pieces):
    blocks = len(pieces)
    part, wide = pieces[0].shape
    full = lambda i, where: (0, 0)
    return pl.pallas_call(
        functools.partial(join_kernel, blocks),
        grid_spec=pltpu.PrefetchScalarGridSpec(
            num_scalar_prefetch=1,
            grid=(1,),
            in_specs=[pl.BlockSpec((part, wide), full)] * blocks,
            out_specs=pl.BlockSpec((part, wide * blocks), full),
        ),
        out_shape=jax.ShapeDtypeStruct((part, wide * blocks), jnp.bfloat16),
        cost_estimate=pl.CostEstimate(
            flops=0, bytes_accessed=4 * part * wide * blocks, transcendentals=0
        ),
    )(where, *pieces)


def emit_kernel(flip, *refs):
    refs[-1][0] = flip[...].T


def emit(flip, layer, stacked):
    hidden, width = flip.shape
    step = 256
    in_specs = [pl.BlockSpec((hidden, step), lambda r: (0, r))]
    args = [flip]
    aliases = {}
    if stacked is not None:
        in_specs.append(pl.BlockSpec(memory_space=pl.ANY))
        args.append(stacked)
        aliases = {1: 0}
    return pl.pallas_call(
        emit_kernel,
        grid=(width // step,),
        in_specs=in_specs,
        out_specs=pl.BlockSpec((1, step, hidden), lambda r: (layer, r, 0)),
        out_shape=jax.ShapeDtypeStruct((2, width, hidden), jnp.bfloat16),
        input_output_aliases=aliases,
        cost_estimate=pl.CostEstimate(
            flops=0, bytes_accessed=4 * hidden * width, transcendentals=0
        ),
    )(*args)


def body(tokens, gate_weight, up_weight, down_weight, in_gain, out_gain):
    groups = lax.axis_size("fs")
    halves = lax.axis_size("grp")
    block_width = gate_weight.shape[2] // groups
    model_width = tokens.shape[1]
    if block_width % (16 * halves) or gate_weight.shape[1] % 128 or gate_weight.shape[2] % 128 or model_width % 256:
        return body_plain(tokens, gate_weight, up_weight, down_weight, in_gain, out_gain)
    rows_mine = tokens.shape[0] // groups
    here = lax.axis_index("fs")
    where = jnp.stack([here, lax.axis_index("grp")]).astype(jnp.int32)
    gain_column = in_gain[:, :, None]
    contract_last = (((1,), (1,)), ((), ()))
    flips = []
    for layer in range(2):
        mats = []
        for weight, gain in ((gate_weight, gain_column), (up_weight, gain_column), (down_weight, None)):
            pieces = list(prepare(where, weight, gain, layer, groups, halves))
            for shift in range(1, groups):
                ring = [(k, (k + shift) % groups) for k in range(groups)]
                pieces[shift] = lax.ppermute(pieces[shift], "fs", ring)
            mats.append(lax.all_gather(join(where, pieces), ("tp", "grp"), axis=0, tiled=True))
        flips.append(mats)
    residual = lax.dynamic_slice_in_dim(tokens, here * rows_mine, rows_mine, 0).astype(jnp.float32)
    normed = normalize(tokens.astype(jnp.float32)).astype(jnp.bfloat16)
    stacked = [None, None, None]
    for layer in range(2):
        gate_flip, up_flip, down_flip = flips[layer]
        stacked = [emit(flip, layer, held) for flip, held in zip(flips[layer], stacked)]
        if layer:
            normed = lax.all_gather(normed, "fs", axis=0, tiled=True)
        gate_act = lax.dot_general(normed, gate_flip, contract_last, preferred_element_type=jnp.float32)
        up_act = lax.dot_general(normed, up_flip, contract_last, preferred_element_type=jnp.float32)
        hidden = (jax.nn.silu(gate_act) * up_act).astype(jnp.bfloat16)
        mixed = lax.psum_scatter(
            jnp.dot(hidden, down_flip, preferred_element_type=jnp.float32),
            "fs",
            scatter_dimension=0,
            tiled=True,
        )
        rounded_state = (residual + 0.5 * out_gain[layer] * normalize(mixed)).astype(jnp.bfloat16)
        residual = rounded_state.astype(jnp.float32)
        normed = normalize(residual).astype(jnp.bfloat16)
    return (*stacked, rounded_state)


def solution(mesh):
    in_specs = (
        P(("grp", "tp"), None),
        P(None, "fs", "tp"),
        P(None, "fs", "tp"),
        P(None, "fs", "tp"),
        P(None, "fs"),
        P(),
    )
    out_specs = (
        P("grp", None, "fs"),
        P("grp", None, "fs"),
        P("grp", None, "fs"),
        P(("grp", "tp", "fs"), None),
    )
    return jax.shard_map(body, mesh=mesh, in_specs=in_specs, out_specs=out_specs, check_vma=False)
```

```python
import functools

import jax
import jax.numpy as jnp
from jax import lax
from jax.experimental import pallas as pl
from jax.experimental.pallas import tpu as pltpu
from jax.sharding import PartitionSpec as P

EPS = 1e-06


def normalize(rows):
    return rows * lax.rsqrt(jnp.mean(rows * rows, axis=-1, keepdims=True) + EPS)


def body_plain(tokens, gate_weight, up_weight, down_weight, in_gain, out_gain):
    groups = lax.axis_size("fs")
    rows_all = tokens.shape[0]
    rows_mine = rows_all // groups
    model_width = tokens.shape[1]
    local_rows = gate_weight.shape[1]
    block_width = gate_weight.shape[2] // groups
    residual = lax.dynamic_slice_in_dim(
        tokens, lax.axis_index("fs") * rows_mine, rows_mine, 0
    ).astype(jnp.float32)
    normed = normalize(tokens.astype(jnp.float32)).astype(jnp.bfloat16)
    gates = []
    ups = []
    downs = []
    rounded_state = tokens
    contract_last = (((1,), (1,)), ((), ()))
    for section_idx in range(2):
        scale = in_gain[section_idx][:, None]
        gate_rounded = (scale * gate_weight[section_idx]).astype(jnp.bfloat16)
        up_rounded = (scale * up_weight[section_idx]).astype(jnp.bfloat16)
        down_rounded = down_weight[section_idx].astype(jnp.bfloat16)
        flipped = [
            w.T.reshape(groups, block_width, local_rows)
            for w in (gate_rounded, up_rounded, down_rounded)
        ]
        arrived = (
            lax.all_to_all(flipped[0], "fs", split_axis=0, concat_axis=2, tiled=True),
            lax.all_to_all(flipped[1], "fs", split_axis=0, concat_axis=2, tiled=True),
            lax.all_to_all(flipped[2], "fs", split_axis=0, concat_axis=2, tiled=True),
        )
        thin_rows = [w.reshape(block_width, model_width) for w in arrived]
        sampler_mats = (
            lax.all_gather(thin_rows[0], "tp", axis=0, tiled=True),
            lax.all_gather(thin_rows[1], "tp", axis=0, tiled=True),
            lax.all_gather(thin_rows[2], "tp", axis=0, tiled=True),
        )
        gate_flip, up_flip, down_flip = (sampler_mats[0], sampler_mats[1], sampler_mats[2])
        gates.append(gate_flip.T)
        ups.append(up_flip.T)
        downs.append(down_flip.T)

        def hidden_of(row_block):
            gate_act = lax.dot_general(
                row_block, gate_flip, contract_last, preferred_element_type=jnp.float32
            )
            up_act = lax.dot_general(
                row_block, up_flip, contract_last, preferred_element_type=jnp.float32
            )
            return (jax.nn.silu(gate_act) * up_act).astype(jnp.bfloat16)

        if section_idx == 0:
            hidden = hidden_of(normed)
        else:
            hidden = hidden_of(lax.all_gather(normed, "fs", axis=0, tiled=True))
        mixed = lax.psum_scatter(
            jnp.dot(hidden, down_flip, preferred_element_type=jnp.float32),
            "fs",
            scatter_dimension=0,
            tiled=True,
        )
        rounded_state = (residual + 0.5 * out_gain[section_idx] * normalize(mixed)).astype(
            jnp.bfloat16
        )
        if section_idx == 0:
            residual = rounded_state.astype(jnp.float32)
            normed = normalize(residual).astype(jnp.bfloat16)
    return (jnp.stack(gates), jnp.stack(ups), jnp.stack(downs), rounded_state)


def prep_kernel(blocks, width, part, scaled, where, *refs):
    if scaled:
        gain, weight, out, flip = refs
        rows = weight[0] * gain[0]
    else:
        weight, out, flip = refs
        rows = weight[0]
    flip[...] = rows.astype(jnp.bfloat16).T
    skip = where[0] * part if part < width else 0
    for target in range(blocks):
        start = pl.multiple_of(target * width + skip, 16)
        out[target] = flip[pl.ds(start, part), :]


def prepare(where, weight, gain, layer, blocks, halves):
    _, rows, cols = weight.shape
    width = cols // blocks
    part = width // halves
    step = 256 if rows % 256 == 0 else rows
    in_specs = [pl.BlockSpec((1, step, cols), lambda r, where: (layer, r, 0))]
    args = [weight]
    if gain is not None:
        in_specs.insert(0, pl.BlockSpec((1, step, 1), lambda r, where: (layer, r, 0)))
        args.insert(0, gain)
    return pl.pallas_call(
        functools.partial(prep_kernel, blocks, width, part, gain is not None),
        grid_spec=pltpu.PrefetchScalarGridSpec(
            num_scalar_prefetch=1,
            grid=(rows // step,),
            in_specs=in_specs,
            out_specs=pl.BlockSpec((blocks, part, step), lambda r, where: (0, 0, r)),
            scratch_shapes=[pltpu.VMEM((cols, step), jnp.bfloat16)],
        ),
        out_shape=jax.ShapeDtypeStruct((blocks, part, rows), jnp.bfloat16),
        cost_estimate=pl.CostEstimate(
            flops=rows * cols, bytes_accessed=rows * cols * 5, transcendentals=0
        ),
    )(where, *args)


def spread_kernel(blocks, *refs):
    sources, full = refs[:3], refs[3:6]
    own, (own_sem, send_sem, recv_sem) = refs[6:9], refs[9:]
    y, z, t = lax.axis_index("grp"), lax.axis_index("fs"), lax.axis_index("tp")
    x, c = t // 2, lax.rem(t, 2)
    other_y, other_x, other_c = 1 - y, (1 - x) * 2 + c, x * 2 + (1 - c)
    wide = sources[0].shape[-1]
    partners = [{"fs": lax.rem(z + shift, blocks)} for shift in range(1, blocks)]
    partners += [{"tp": other_x}, {"tp": other_c}, {"grp": other_y}]

    barrier = pltpu.get_barrier_semaphore()
    for partner in partners:
        pl.semaphore_signal(barrier, inc=1, device_id=partner, device_id_type=pl.DeviceIdType.MESH)
    pl.semaphore_wait(barrier, len(partners))

    def columns(source):
        return pl.ds(pl.multiple_of(source * wide, 128), wide)

    def place(m, column, half, source):
        cols = columns(source)
        if m == 2:
            return full[m].at[column, :, :, cols]
        return full[m].at[column, half, :, cols]

    def rows_of(m, column, half):
        if m == 2:
            return full[m].at[column]
        return full[m].at[column, half]

    def origin(m, target):
        return sources[m].at[target]

    names = []
    sent = []

    def slot(name):
        if name not in names:
            names.append(name)
        return names.index(name)

    def send(name, source, target, device):
        k = slot(name)
        copy = pltpu.make_async_remote_copy(
            src_ref=source,
            dst_ref=target,
            send_sem=send_sem.at[k],
            recv_sem=recv_sem.at[k],
            device_id=device,
            device_id_type=pl.DeviceIdType.MESH,
        )
        copy.start()
        sent.append(copy)

    def arrived(name, landed, device):
        k = slot(name)
        pltpu.make_async_remote_copy(
            src_ref=landed,
            dst_ref=landed,
            send_sem=send_sem.at[k],
            recv_sem=recv_sem.at[k],
            device_id=device,
            device_id_type=pl.DeviceIdType.MESH,
        ).wait_recv()

    to_x, to_c, to_y = {"tp": other_x}, {"tp": other_c}, {"grp": other_y}
    fetch = []
    for m in range(3):
        for shift in range(1, blocks):
            target = lax.rem(z + shift, blocks)
            send(("z", m, shift), origin(m, target), place(m, t, y, z), {"fs": target})
        mine = origin(m, z)
        send(("x", m, 0), mine, place(m, t, y, z), to_x)
        if m < 2:
            send(("y", m, 0, 0), mine, place(m, t, y, z), to_y)
        copy = pltpu.make_async_copy(mine, own[m], own_sem.at[m])
        copy.start()
        fetch.append(copy)
    kept = []
    for m in range(3):
        fetch[m].wait()
        copy = pltpu.make_async_copy(own[m], place(m, t, y, z), own_sem.at[3 + m])
        copy.start()
        kept.append(copy)

    def relay(m, shift):
        source = lax.rem(z + blocks - shift, blocks)
        arrived(("x", m, shift), place(m, other_x, y, source), to_x)
        if m < 2:
            spot = place(m, other_x, y, source)
            send(("y", m, 1, shift), spot, spot, to_y)

    for m in range(3):
        for shift in range(1, blocks):
            source = lax.rem(z + blocks - shift, blocks)
            spot = place(m, t, y, source)
            arrived(("z", m, shift), spot, {"fs": source})
            send(("x", m, shift), spot, spot, to_x)
            if m < 2:
                send(("y", m, 0, shift), spot, spot, to_y)
            relay(m, shift - 1)
        kept[m].wait()
        send(("c", m, 0, 0), rows_of(m, t, y), rows_of(m, t, y), to_c)
        relay(m, blocks - 1)
        send(("c", m, 1, 0), rows_of(m, other_x, y), rows_of(m, other_x, y), to_c)
    for m in range(2):
        for far, column in ((0, t), (1, other_x)):
            for shift in range(blocks):
                source = lax.rem(z + blocks - shift, blocks)
                arrived(("y", m, far, shift), place(m, column, other_y, source), to_y)
            rows = rows_of(m, column, other_y)
            send(("c", m, far, 1), rows, rows, to_c)
    other_both = (1 - x) * 2 + (1 - c)
    for m in range(3):
        for far, column in ((0, other_c), (1, other_both)):
            arrived(("c", m, far, 0), rows_of(m, column, y), to_c)
            if m < 2:
                arrived(("c", m, far, 1), rows_of(m, column, other_y), to_c)
    for copy in sent:
        copy.wait_send()


def spread(sources, layer, blocks, columns):
    halves, part = 2, sources[0].shape[1]
    rows = sources[0].shape[2]
    sources = [sources[0], sources[1], sources[2].reshape(blocks, halves, part, rows)]
    count = 3 * (blocks - 1) + 3 * blocks + 4 * blocks + 10
    shape = (columns, halves, part, rows * blocks)
    moved = columns * halves * part * rows * blocks * 2
    return pl.pallas_call(
        functools.partial(spread_kernel, blocks),
        in_specs=[pl.BlockSpec(memory_space=pl.ANY)] * 3,
        out_specs=[pl.BlockSpec(memory_space=pl.ANY)] * 3,
        out_shape=[jax.ShapeDtypeStruct(shape, jnp.bfloat16)] * 3,
        scratch_shapes=[
            pltpu.VMEM((part, rows), jnp.bfloat16),
            pltpu.VMEM((part, rows), jnp.bfloat16),
            pltpu.VMEM((halves, part, rows), jnp.bfloat16),
            pltpu.SemaphoreType.DMA((6,)),
            pltpu.SemaphoreType.DMA((count,)),
            pltpu.SemaphoreType.DMA((count,)),
        ],
        compiler_params=pltpu.CompilerParams(collective_id=layer, has_side_effects=True),
        cost_estimate=pl.CostEstimate(flops=0, bytes_accessed=moved * 40, transcendentals=0),
    )(*sources)


def emit_kernel(flip, *refs):
    refs[-1][0] = flip[...].T


def emit(flip, layer, stacked):
    hidden, width = flip.shape
    step = 256
    in_specs = [pl.BlockSpec((hidden, step), lambda r: (0, r))]
    args = [flip]
    aliases = {}
    if stacked is not None:
        in_specs.append(pl.BlockSpec(memory_space=pl.ANY))
        args.append(stacked)
        aliases = {1: 0}
    return pl.pallas_call(
        emit_kernel,
        grid=(width // step,),
        in_specs=in_specs,
        out_specs=pl.BlockSpec((1, step, hidden), lambda r: (layer, r, 0)),
        out_shape=jax.ShapeDtypeStruct((2, width, hidden), jnp.bfloat16),
        input_output_aliases=aliases,
        cost_estimate=pl.CostEstimate(
            flops=0, bytes_accessed=4 * hidden * width, transcendentals=0
        ),
    )(*args)


def body(tokens, gate_weight, up_weight, down_weight, in_gain, out_gain):
    groups = lax.axis_size("fs")
    halves = lax.axis_size("grp")
    block_width = gate_weight.shape[2] // groups
    model_width = tokens.shape[1]
    columns = lax.axis_size("tp")
    odd = block_width % 32 or gate_weight.shape[1] % 128 or gate_weight.shape[2] % 128
    if odd or model_width % 256 or halves != 2 or columns != 4:
        return body_plain(tokens, gate_weight, up_weight, down_weight, in_gain, out_gain)
    rows_mine = tokens.shape[0] // groups
    here = lax.axis_index("fs")
    where = lax.axis_index("grp")[None].astype(jnp.int32)
    gain_column = in_gain[:, :, None]
    contract_last = (((1,), (1,)), ((), ()))
    flips = []
    for layer in range(2):
        pieces = [
            prepare(where, gate_weight, gain_column, layer, groups, halves),
            prepare(where, up_weight, gain_column, layer, groups, halves),
            prepare(where, down_weight, None, layer, groups, 1),
        ]
        whole = spread(pieces, layer, groups, columns)
        flips.append([mat.reshape(columns * block_width, model_width) for mat in whole])
    residual = lax.dynamic_slice_in_dim(tokens, here * rows_mine, rows_mine, 0).astype(jnp.float32)
    normed = normalize(tokens.astype(jnp.float32)).astype(jnp.bfloat16)
    stacked = [None, None, None]
    for layer in range(2):
        gate_flip, up_flip, down_flip = flips[layer]
        stacked = [emit(flip, layer, held) for flip, held in zip(flips[layer], stacked)]
        if layer:
            normed = lax.all_gather(normed, "fs", axis=0, tiled=True)
        gate_act = lax.dot_general(normed, gate_flip, contract_last, preferred_element_type=jnp.float32)
        up_act = lax.dot_general(normed, up_flip, contract_last, preferred_element_type=jnp.float32)
        hidden = (jax.nn.silu(gate_act) * up_act).astype(jnp.bfloat16)
        mixed = lax.psum_scatter(
            jnp.dot(hidden, down_flip, preferred_element_type=jnp.float32).astype(jnp.bfloat16),
            "fs",
            scatter_dimension=0,
            tiled=True,
        ).astype(jnp.float32)
        rounded_state = (residual + 0.5 * out_gain[layer] * normalize(mixed)).astype(jnp.bfloat16)
        residual = rounded_state.astype(jnp.float32)
        normed = normalize(residual).astype(jnp.bfloat16)
    return (*stacked, rounded_state)


def solution(mesh):
    in_specs = (
        P(("grp", "tp"), None),
        P(None, "fs", "tp"),
        P(None, "fs", "tp"),
        P(None, "fs", "tp"),
        P(None, "fs"),
        P(),
    )
    out_specs = (
        P("grp", None, "fs"),
        P("grp", None, "fs"),
        P("grp", None, "fs"),
        P(("grp", "tp", "fs"), None),
    )
    return jax.shard_map(body, mesh=mesh, in_specs=in_specs, out_specs=out_specs, check_vma=False)
```

```python
import functools

import jax
import jax.numpy as jnp
from jax import lax
from jax.experimental import pallas as pl
from jax.experimental.pallas import tpu as pltpu
from jax.sharding import PartitionSpec as P

EPS = 1e-06


def normalize(rows):
    return rows * lax.rsqrt(jnp.mean(rows * rows, axis=-1, keepdims=True) + EPS)


def body_plain(tokens, gate_weight, up_weight, down_weight, in_gain, out_gain):
    groups = lax.axis_size("fs")
    rows_all = tokens.shape[0]
    rows_mine = rows_all // groups
    model_width = tokens.shape[1]
    local_rows = gate_weight.shape[1]
    block_width = gate_weight.shape[2] // groups
    residual = lax.dynamic_slice_in_dim(
        tokens, lax.axis_index("fs") * rows_mine, rows_mine, 0
    ).astype(jnp.float32)
    normed = normalize(tokens.astype(jnp.float32)).astype(jnp.bfloat16)
    gates = []
    ups = []
    downs = []
    rounded_state = tokens
    contract_last = (((1,), (1,)), ((), ()))
    for section_idx in range(2):
        scale = in_gain[section_idx][:, None]
        gate_rounded = (scale * gate_weight[section_idx]).astype(jnp.bfloat16)
        up_rounded = (scale * up_weight[section_idx]).astype(jnp.bfloat16)
        down_rounded = down_weight[section_idx].astype(jnp.bfloat16)
        flipped = [
            w.T.reshape(groups, block_width, local_rows)
            for w in (gate_rounded, up_rounded, down_rounded)
        ]
        arrived = (
            lax.all_to_all(flipped[0], "fs", split_axis=0, concat_axis=2, tiled=True),
            lax.all_to_all(flipped[1], "fs", split_axis=0, concat_axis=2, tiled=True),
            lax.all_to_all(flipped[2], "fs", split_axis=0, concat_axis=2, tiled=True),
        )
        thin_rows = [w.reshape(block_width, model_width) for w in arrived]
        sampler_mats = (
            lax.all_gather(thin_rows[0], "tp", axis=0, tiled=True),
            lax.all_gather(thin_rows[1], "tp", axis=0, tiled=True),
            lax.all_gather(thin_rows[2], "tp", axis=0, tiled=True),
        )
        gate_flip, up_flip, down_flip = (sampler_mats[0], sampler_mats[1], sampler_mats[2])
        gates.append(gate_flip.T)
        ups.append(up_flip.T)
        downs.append(down_flip.T)

        def hidden_of(row_block):
            gate_act = lax.dot_general(
                row_block, gate_flip, contract_last, preferred_element_type=jnp.float32
            )
            up_act = lax.dot_general(
                row_block, up_flip, contract_last, preferred_element_type=jnp.float32
            )
            return (jax.nn.silu(gate_act) * up_act).astype(jnp.bfloat16)

        if section_idx == 0:
            hidden = hidden_of(normed)
        else:
            hidden = hidden_of(lax.all_gather(normed, "fs", axis=0, tiled=True))
        mixed = lax.psum_scatter(
            jnp.dot(hidden, down_flip, preferred_element_type=jnp.float32),
            "fs",
            scatter_dimension=0,
            tiled=True,
        )
        rounded_state = (residual + 0.5 * out_gain[section_idx] * normalize(mixed)).astype(
            jnp.bfloat16
        )
        if section_idx == 0:
            residual = rounded_state.astype(jnp.float32)
            normed = normalize(residual).astype(jnp.bfloat16)
    return (jnp.stack(gates), jnp.stack(ups), jnp.stack(downs), rounded_state)


COVER = 3


def prep_kernel(blocks, width, part, scaled, where, *refs):
    if scaled:
        gain, weight, out, flip = refs
        rows = weight[0] * gain[0]
    else:
        weight, out, flip = refs
        rows = weight[0]
    flip[...] = rows.astype(jnp.bfloat16).T
    skip = where[0] * part if part < width else 0
    for target in range(blocks):
        start = pl.multiple_of(target * width + skip, 16)
        out[target] = flip[pl.ds(start, part), :]


def prepare(where, weight, gain, layer, blocks, halves):
    _, rows, cols = weight.shape
    width = cols // blocks
    part = width // halves
    step = 256 if rows % 256 == 0 else rows
    in_specs = [pl.BlockSpec((1, step, cols), lambda r, where: (layer, r, 0))]
    args = [weight]
    if gain is not None:
        in_specs.insert(0, pl.BlockSpec((1, step, 1), lambda r, where: (layer, r, 0)))
        args.insert(0, gain)
    return pl.pallas_call(
        functools.partial(prep_kernel, blocks, width, part, gain is not None),
        grid_spec=pltpu.PrefetchScalarGridSpec(
            num_scalar_prefetch=1,
            grid=(rows // step,),
            in_specs=in_specs,
            out_specs=pl.BlockSpec((blocks, part, step), lambda r, where: (0, 0, r)),
            scratch_shapes=[pltpu.VMEM((cols, step), jnp.bfloat16)],
        ),
        out_shape=jax.ShapeDtypeStruct((blocks, part, rows), jnp.bfloat16),
        cost_estimate=pl.CostEstimate(
            flops=rows * cols, bytes_accessed=rows * cols * 5, transcendentals=0
        ),
    )(where, *args)


def spread_kernel(blocks, *refs):
    sources, full = refs[:3], refs[3:6]
    own, (own_sem, send_sem, recv_sem) = refs[6:9], refs[9:]
    y, z, t = lax.axis_index("grp"), lax.axis_index("fs"), lax.axis_index("tp")
    x, c = t // 2, lax.rem(t, 2)
    other_y, other_x, other_c = 1 - y, (1 - x) * 2 + c, x * 2 + (1 - c)
    wide = sources[0].shape[-1]
    partners = [{"fs": lax.rem(z + shift, blocks)} for shift in range(1, blocks)]
    partners += [{"tp": other_x}, {"tp": other_c}, {"grp": other_y}]

    barrier = pltpu.get_barrier_semaphore()
    for partner in partners:
        pl.semaphore_signal(barrier, inc=1, device_id=partner, device_id_type=pl.DeviceIdType.MESH)
    pl.semaphore_wait(barrier, len(partners))

    def columns(source):
        return pl.ds(pl.multiple_of(source * wide, 128), wide)

    def place(m, column, half, source):
        cols = columns(source)
        if m == 2:
            return full[m].at[column, :, :, cols]
        return full[m].at[column, half, :, cols]

    def rows_of(m, column, half):
        if m == 2:
            return full[m].at[column]
        return full[m].at[column, half]

    def origin(m, target):
        return sources[m].at[target]

    names = []
    sent = []

    def slot(name):
        if name not in names:
            names.append(name)
        return names.index(name)

    def send(name, source, target, device):
        k = slot(name)
        copy = pltpu.make_async_remote_copy(
            src_ref=source,
            dst_ref=target,
            send_sem=send_sem.at[k],
            recv_sem=recv_sem.at[k],
            device_id=device,
            device_id_type=pl.DeviceIdType.MESH,
        )
        copy.start()
        sent.append(copy)

    def arrived(name, landed, device):
        k = slot(name)
        pltpu.make_async_remote_copy(
            src_ref=landed,
            dst_ref=landed,
            send_sem=send_sem.at[k],
            recv_sem=recv_sem.at[k],
            device_id=device,
            device_id_type=pl.DeviceIdType.MESH,
        ).wait_recv()

    to_x, to_c, to_y = {"tp": other_x}, {"tp": other_c}, {"grp": other_y}
    fetch = []
    for m in range(3):
        for shift in range(1, blocks):
            target = lax.rem(z + shift, blocks)
            send(("z", m, shift), origin(m, target), place(m, t, y, z), {"fs": target})
        mine = origin(m, z)
        send(("x", m, 0), mine, place(m, t, y, z), to_x)
        if m < 2:
            send(("y", m, 0, 0), mine, place(m, t, y, z), to_y)
        copy = pltpu.make_async_copy(mine, own[m], own_sem.at[m])
        copy.start()
        fetch.append(copy)
    kept = []
    for m in range(3):
        fetch[m].wait()
        copy = pltpu.make_async_copy(own[m], place(m, t, y, z), own_sem.at[3 + m])
        copy.start()
        kept.append(copy)

    def relay(m, shift):
        source = lax.rem(z + blocks - shift, blocks)
        arrived(("x", m, shift), place(m, other_x, y, source), to_x)
        if m < 2:
            spot = place(m, other_x, y, source)
            send(("y", m, 1, shift), spot, spot, to_y)

    for m in range(3):
        for shift in range(1, blocks):
            source = lax.rem(z + blocks - shift, blocks)
            spot = place(m, t, y, source)
            arrived(("z", m, shift), spot, {"fs": source})
            send(("x", m, shift), spot, spot, to_x)
            if m < 2:
                send(("y", m, 0, shift), spot, spot, to_y)
            relay(m, shift - 1)
        kept[m].wait()
        send(("c", m, 0, 0), rows_of(m, t, y), rows_of(m, t, y), to_c)
        relay(m, blocks - 1)
        send(("c", m, 1, 0), rows_of(m, other_x, y), rows_of(m, other_x, y), to_c)
    for m in range(2):
        for far, column in ((0, t), (1, other_x)):
            for shift in range(blocks):
                source = lax.rem(z + blocks - shift, blocks)
                arrived(("y", m, far, shift), place(m, column, other_y, source), to_y)
            rows = rows_of(m, column, other_y)
            send(("c", m, far, 1), rows, rows, to_c)
    other_both = (1 - x) * 2 + (1 - c)
    for m in range(3):
        for far, column in ((0, other_c), (1, other_both)):
            arrived(("c", m, far, 0), rows_of(m, column, y), to_c)
            if m < 2:
                arrived(("c", m, far, 1), rows_of(m, column, other_y), to_c)
    for copy in sent:
        copy.wait_send()


def spread(sources, layer, blocks, columns):
    halves, part = 2, sources[0].shape[1]
    rows = sources[0].shape[2]
    sources = [sources[0], sources[1], sources[2].reshape(blocks, halves, part, rows)]
    count = 3 * (blocks - 1) + 3 * blocks + 4 * blocks + 10
    shape = (columns, halves, part, rows * blocks)
    moved = columns * halves * part * rows * blocks * 2
    return pl.pallas_call(
        functools.partial(spread_kernel, blocks),
        in_specs=[pl.BlockSpec(memory_space=pl.ANY)] * 3,
        out_specs=[pl.BlockSpec(memory_space=pl.ANY)] * 3,
        out_shape=[jax.ShapeDtypeStruct(shape, jnp.bfloat16)] * 3,
        scratch_shapes=[
            pltpu.VMEM((part, rows), jnp.bfloat16),
            pltpu.VMEM((part, rows), jnp.bfloat16),
            pltpu.VMEM((halves, part, rows), jnp.bfloat16),
            pltpu.SemaphoreType.DMA((6,)),
            pltpu.SemaphoreType.DMA((count,)),
            pltpu.SemaphoreType.DMA((count,)),
        ],
        compiler_params=pltpu.CompilerParams(collective_id=layer, has_side_effects=True),
        cost_estimate=pl.CostEstimate(flops=0, bytes_accessed=moved * 40, transcendentals=0),
    )(*sources)


def emit_kernel(flip, *refs):
    refs[-1][0] = flip[...].T


def emit(flip, layer, stacked):
    hidden, width = flip.shape
    step = 256
    in_specs = [pl.BlockSpec((hidden, step), lambda r: (0, r))]
    args = [flip]
    aliases = {}
    if stacked is not None:
        in_specs.append(pl.BlockSpec(memory_space=pl.ANY))
        args.append(stacked)
        aliases = {1: 0}
    return pl.pallas_call(
        emit_kernel,
        grid=(width // step,),
        in_specs=in_specs,
        out_specs=pl.BlockSpec((1, step, hidden), lambda r: (layer, r, 0)),
        out_shape=jax.ShapeDtypeStruct((2, width, hidden), jnp.bfloat16),
        input_output_aliases=aliases,
        cost_estimate=pl.CostEstimate(
            flops=0, bytes_accessed=4 * hidden * width, transcendentals=0
        ),
    )(*args)


def body(tokens, gate_weight, up_weight, down_weight, in_gain, out_gain):
    groups = lax.axis_size("fs")
    halves = lax.axis_size("grp")
    block_width = gate_weight.shape[2] // groups
    model_width = tokens.shape[1]
    columns = lax.axis_size("tp")
    odd = block_width % 32 or gate_weight.shape[1] % 128 or gate_weight.shape[2] % 128
    if odd or model_width % 256 or halves != 2 or columns != 4:
        return body_plain(tokens, gate_weight, up_weight, down_weight, in_gain, out_gain)
    rows_mine = tokens.shape[0] // groups
    here = lax.axis_index("fs")
    where = lax.axis_index("grp")[None].astype(jnp.int32)
    gain_column = in_gain[:, :, None]
    contract_last = (((1,), (1,)), ((), ()))
    pieces = [
        [
            prepare(where, gate_weight, gain_column, layer, groups, halves),
            prepare(where, up_weight, gain_column, layer, groups, halves),
            prepare(where, down_weight, None, layer, groups, 1),
        ]
        for layer in range(2)
    ]
    residual = lax.dynamic_slice_in_dim(tokens, here * rows_mine, rows_mine, 0).astype(jnp.float32)
    normed = normalize(tokens.astype(jnp.float32)).astype(jnp.bfloat16)
    stacked = [None, None, None]
    whole = spread(pieces[0], 0, groups, columns)
    for layer in range(2):
        flips = [mat.reshape(columns * block_width, model_width) for mat in whole]
        gate_flip, up_flip, down_flip = flips
        gate_act = lax.dot_general(normed, gate_flip, contract_last, preferred_element_type=jnp.float32)
        up_act = lax.dot_general(normed, up_flip, contract_last, preferred_element_type=jnp.float32)
        hidden = (jax.nn.silu(gate_act) * up_act).astype(jnp.bfloat16)
        partial = jnp.dot(hidden, down_flip, preferred_element_type=jnp.float32).astype(jnp.bfloat16)
        if layer == 0:
            partial, *later = lax.optimization_barrier((partial, *pieces[1]))
            whole = spread(later, 1, groups, columns)
        mixed = lax.psum_scatter(partial, "fs", scatter_dimension=0, tiled=True)
        if layer == 0:
            mixed, *whole = lax.optimization_barrier((mixed, *whole))
        mixed = mixed.astype(jnp.float32)
        rounded_state = (residual + 0.5 * out_gain[layer] * normalize(mixed)).astype(jnp.bfloat16)
        if layer == 0:
            residual = rounded_state.astype(jnp.float32)
            normed = normalize(residual).astype(jnp.bfloat16)
            normed, *flips = lax.optimization_barrier((normed, *flips))
            normed = lax.all_gather(normed, "fs", axis=0, tiled=True)
            stacked = [emit(flip, 0, None) for flip in flips]
            normed, *stacked[:COVER] = lax.optimization_barrier((normed, *stacked[:COVER]))
        else:
            stacked = [emit(flip, 1, held) for flip, held in zip(flips, stacked)]
    return (*stacked, rounded_state)


def solution(mesh):
    in_specs = (
        P(("grp", "tp"), None),
        P(None, "fs", "tp"),
        P(None, "fs", "tp"),
        P(None, "fs", "tp"),
        P(None, "fs"),
        P(),
    )
    out_specs = (
        P("grp", None, "fs"),
        P("grp", None, "fs"),
        P("grp", None, "fs"),
        P(("grp", "tp", "fs"), None),
    )
    return jax.shard_map(body, mesh=mesh, in_specs=in_specs, out_specs=out_specs, check_vma=False)
```

```python
import functools

import jax
import jax.numpy as jnp
from jax import lax
from jax.experimental import pallas as pl
from jax.experimental.pallas import tpu as pltpu
from jax.sharding import PartitionSpec as P

EPS = 1e-06


def normalize(rows):
    return rows * lax.rsqrt(jnp.mean(rows * rows, axis=-1, keepdims=True) + EPS)


def body_plain(tokens, gate_weight, up_weight, down_weight, in_gain, out_gain):
    groups = lax.axis_size("fs")
    rows_all = tokens.shape[0]
    rows_mine = rows_all // groups
    model_width = tokens.shape[1]
    local_rows = gate_weight.shape[1]
    block_width = gate_weight.shape[2] // groups
    residual = lax.dynamic_slice_in_dim(
        tokens, lax.axis_index("fs") * rows_mine, rows_mine, 0
    ).astype(jnp.float32)
    normed = normalize(tokens.astype(jnp.float32)).astype(jnp.bfloat16)
    gates = []
    ups = []
    downs = []
    rounded_state = tokens
    contract_last = (((1,), (1,)), ((), ()))
    for section_idx in range(2):
        scale = in_gain[section_idx][:, None]
        gate_rounded = (scale * gate_weight[section_idx]).astype(jnp.bfloat16)
        up_rounded = (scale * up_weight[section_idx]).astype(jnp.bfloat16)
        down_rounded = down_weight[section_idx].astype(jnp.bfloat16)
        flipped = [
            w.T.reshape(groups, block_width, local_rows)
            for w in (gate_rounded, up_rounded, down_rounded)
        ]
        arrived = (
            lax.all_to_all(flipped[0], "fs", split_axis=0, concat_axis=2, tiled=True),
            lax.all_to_all(flipped[1], "fs", split_axis=0, concat_axis=2, tiled=True),
            lax.all_to_all(flipped[2], "fs", split_axis=0, concat_axis=2, tiled=True),
        )
        thin_rows = [w.reshape(block_width, model_width) for w in arrived]
        sampler_mats = (
            lax.all_gather(thin_rows[0], "tp", axis=0, tiled=True),
            lax.all_gather(thin_rows[1], "tp", axis=0, tiled=True),
            lax.all_gather(thin_rows[2], "tp", axis=0, tiled=True),
        )
        gate_flip, up_flip, down_flip = (sampler_mats[0], sampler_mats[1], sampler_mats[2])
        gates.append(gate_flip.T)
        ups.append(up_flip.T)
        downs.append(down_flip.T)

        def hidden_of(row_block):
            gate_act = lax.dot_general(
                row_block, gate_flip, contract_last, preferred_element_type=jnp.float32
            )
            up_act = lax.dot_general(
                row_block, up_flip, contract_last, preferred_element_type=jnp.float32
            )
            return (jax.nn.silu(gate_act) * up_act).astype(jnp.bfloat16)

        if section_idx == 0:
            hidden = hidden_of(normed)
        else:
            hidden = hidden_of(lax.all_gather(normed, "fs", axis=0, tiled=True))
        mixed = lax.psum_scatter(
            jnp.dot(hidden, down_flip, preferred_element_type=jnp.float32),
            "fs",
            scatter_dimension=0,
            tiled=True,
        )
        rounded_state = (residual + 0.5 * out_gain[section_idx] * normalize(mixed)).astype(
            jnp.bfloat16
        )
        if section_idx == 0:
            residual = rounded_state.astype(jnp.float32)
            normed = normalize(residual).astype(jnp.bfloat16)
    return (jnp.stack(gates), jnp.stack(ups), jnp.stack(downs), rounded_state)


def prep_kernel(blocks, width, part, scaled, where, *refs):
    if scaled:
        gain, weight, out, flip = refs
        rows = weight[0] * gain[0]
    else:
        weight, out, flip = refs
        rows = weight[0]
    flip[...] = rows.astype(jnp.bfloat16).T
    skip = where[0] * part if part < width else 0
    for target in range(blocks):
        start = pl.multiple_of(target * width + skip, 16)
        out[target] = flip[pl.ds(start, part), :]


def prepare(where, weight, gain, layer, blocks, halves):
    _, rows, cols = weight.shape
    width = cols // blocks
    part = width // halves
    step = 256 if rows % 256 == 0 else rows
    in_specs = [pl.BlockSpec((1, step, cols), lambda r, where: (layer, r, 0))]
    args = [weight]
    if gain is not None:
        in_specs.insert(0, pl.BlockSpec((1, step, 1), lambda r, where: (layer, r, 0)))
        args.insert(0, gain)
    return pl.pallas_call(
        functools.partial(prep_kernel, blocks, width, part, gain is not None),
        grid_spec=pltpu.PrefetchScalarGridSpec(
            num_scalar_prefetch=1,
            grid=(rows // step,),
            in_specs=in_specs,
            out_specs=pl.BlockSpec((blocks, part, step), lambda r, where: (0, 0, r)),
            scratch_shapes=[pltpu.VMEM((cols, step), jnp.bfloat16)],
        ),
        out_shape=jax.ShapeDtypeStruct((blocks, part, rows), jnp.bfloat16),
        cost_estimate=pl.CostEstimate(
            flops=rows * cols, bytes_accessed=rows * cols * 5, transcendentals=0
        ),
    )(where, *args)


def spread_kernel(blocks, split, *refs):
    n = len(split)
    sources, full = refs[:n], refs[n : 2 * n]
    own, (own_sem, send_sem, recv_sem) = refs[2 * n : 3 * n], refs[3 * n :]
    y, z, t = lax.axis_index("grp"), lax.axis_index("fs"), lax.axis_index("tp")
    x, c = t // 2, lax.rem(t, 2)
    other_y, other_x, other_c = 1 - y, (1 - x) * 2 + c, x * 2 + (1 - c)
    wide = sources[0].shape[-1]
    partners = [{"fs": lax.rem(z + shift, blocks)} for shift in range(1, blocks)]
    partners += [{"tp": other_x}, {"tp": other_c}, {"grp": other_y}]

    barrier = pltpu.get_barrier_semaphore()
    for partner in partners:
        pl.semaphore_signal(barrier, inc=1, device_id=partner, device_id_type=pl.DeviceIdType.MESH)
    pl.semaphore_wait(barrier, len(partners))

    def columns(source):
        return pl.ds(pl.multiple_of(source * wide, 128), wide)

    def place(m, column, half, source):
        cols = columns(source)
        if not split[m]:
            return full[m].at[column, :, :, cols]
        return full[m].at[column, half, :, cols]

    def rows_of(m, column, half):
        if not split[m]:
            return full[m].at[column]
        return full[m].at[column, half]

    def origin(m, target):
        return sources[m].at[target]

    names = []
    sent = []

    def slot(name):
        if name not in names:
            names.append(name)
        return names.index(name)

    def send(name, source, target, device):
        k = slot(name)
        copy = pltpu.make_async_remote_copy(
            src_ref=source,
            dst_ref=target,
            send_sem=send_sem.at[k],
            recv_sem=recv_sem.at[k],
            device_id=device,
            device_id_type=pl.DeviceIdType.MESH,
        )
        copy.start()
        sent.append(copy)

    def arrived(name, landed, device):
        k = slot(name)
        pltpu.make_async_remote_copy(
            src_ref=landed,
            dst_ref=landed,
            send_sem=send_sem.at[k],
            recv_sem=recv_sem.at[k],
            device_id=device,
            device_id_type=pl.DeviceIdType.MESH,
        ).wait_recv()

    to_x, to_c, to_y = {"tp": other_x}, {"tp": other_c}, {"grp": other_y}
    fetch = []
    for m in range(n):
        for shift in range(1, blocks):
            target = lax.rem(z + shift, blocks)
            send(("z", m, shift), origin(m, target), place(m, t, y, z), {"fs": target})
        mine = origin(m, z)
        send(("x", m, 0), mine, place(m, t, y, z), to_x)
        if split[m]:
            send(("y", m, 0, 0), mine, place(m, t, y, z), to_y)
        copy = pltpu.make_async_copy(mine, own[m], own_sem.at[m])
        copy.start()
        fetch.append(copy)
    kept = []
    for m in range(n):
        fetch[m].wait()
        copy = pltpu.make_async_copy(own[m], place(m, t, y, z), own_sem.at[n + m])
        copy.start()
        kept.append(copy)

    def relay(m, shift):
        source = lax.rem(z + blocks - shift, blocks)
        arrived(("x", m, shift), place(m, other_x, y, source), to_x)
        if split[m]:
            spot = place(m, other_x, y, source)
            send(("y", m, 1, shift), spot, spot, to_y)

    for m in range(n):
        for shift in range(1, blocks):
            source = lax.rem(z + blocks - shift, blocks)
            spot = place(m, t, y, source)
            arrived(("z", m, shift), spot, {"fs": source})
            send(("x", m, shift), spot, spot, to_x)
            if split[m]:
                send(("y", m, 0, shift), spot, spot, to_y)
            relay(m, shift - 1)
        kept[m].wait()
        send(("c", m, 0, 0), rows_of(m, t, y), rows_of(m, t, y), to_c)
        relay(m, blocks - 1)
        send(("c", m, 1, 0), rows_of(m, other_x, y), rows_of(m, other_x, y), to_c)
    for m in range(n):
        if not split[m]:
            continue
        for far, column in ((0, t), (1, other_x)):
            for shift in range(blocks):
                source = lax.rem(z + blocks - shift, blocks)
                arrived(("y", m, far, shift), place(m, column, other_y, source), to_y)
            rows = rows_of(m, column, other_y)
            send(("c", m, far, 1), rows, rows, to_c)
    other_both = (1 - x) * 2 + (1 - c)
    for m in range(n):
        for far, column in ((0, other_c), (1, other_both)):
            arrived(("c", m, far, 0), rows_of(m, column, y), to_c)
            if split[m]:
                arrived(("c", m, far, 1), rows_of(m, column, other_y), to_c)
    for copy in sent:
        copy.wait_send()


def spread(sources, split, blocks, columns):
    n, halves = len(split), 2
    part, rows = sources[0].shape[1:]
    sources = [
        source if alone else source.reshape(blocks, halves, part, rows)
        for source, alone in zip(sources, split)
    ]
    count = sum(4 * blocks + 1 + (2 * blocks + 2) * alone for alone in split)
    shape = (columns, halves, part, rows * blocks)
    moved = n * columns * halves * part * rows * blocks * 2
    whole = pl.BlockSpec(memory_space=pl.ANY)
    return pl.pallas_call(
        functools.partial(spread_kernel, blocks, split),
        in_specs=[whole] * n,
        out_specs=[whole] * n,
        out_shape=[jax.ShapeDtypeStruct(shape, jnp.bfloat16)] * n,
        scratch_shapes=[pltpu.VMEM(source.shape[1:], jnp.bfloat16) for source in sources]
        + [
            pltpu.SemaphoreType.DMA((2 * n,)),
            pltpu.SemaphoreType.DMA((count,)),
            pltpu.SemaphoreType.DMA((count,)),
        ],
        compiler_params=pltpu.CompilerParams(collective_id=0, has_side_effects=True),
        cost_estimate=pl.CostEstimate(flops=0, bytes_accessed=moved * 13, transcendentals=0),
    )(*sources)


def emit_kernel(flip, *refs):
    refs[-1][0] = flip[...].T


def emit(flip, layer, stacked):
    hidden, width = flip.shape
    step = 256
    in_specs = [pl.BlockSpec((hidden, step), lambda r: (0, r))]
    args = [flip]
    aliases = {}
    if stacked is not None:
        in_specs.append(pl.BlockSpec(memory_space=pl.ANY))
        args.append(stacked)
        aliases = {1: 0}
    return pl.pallas_call(
        emit_kernel,
        grid=(width // step,),
        in_specs=in_specs,
        out_specs=pl.BlockSpec((1, step, hidden), lambda r: (layer, r, 0)),
        out_shape=jax.ShapeDtypeStruct((2, width, hidden), jnp.bfloat16),
        input_output_aliases=aliases,
        cost_estimate=pl.CostEstimate(
            flops=0, bytes_accessed=4 * hidden * width, transcendentals=0
        ),
    )(*args)


def body(tokens, gate_weight, up_weight, down_weight, in_gain, out_gain):
    groups = lax.axis_size("fs")
    halves = lax.axis_size("grp")
    block_width = gate_weight.shape[2] // groups
    model_width = tokens.shape[1]
    columns = lax.axis_size("tp")
    odd = block_width % 32 or gate_weight.shape[1] % 128 or gate_weight.shape[2] % 128
    if odd or model_width % 256 or halves != 2 or columns != 4:
        return body_plain(tokens, gate_weight, up_weight, down_weight, in_gain, out_gain)
    rows_mine = tokens.shape[0] // groups
    here = lax.axis_index("fs")
    where = lax.axis_index("grp")[None].astype(jnp.int32)
    gain_column = in_gain[:, :, None]
    contract_last = (((1,), (1,)), ((), ()))
    pieces = [
        [
            prepare(where, gate_weight, gain_column, layer, groups, halves),
            prepare(where, up_weight, gain_column, layer, groups, halves),
            prepare(where, down_weight, None, layer, groups, 1),
        ]
        for layer in range(2)
    ]
    residual = lax.dynamic_slice_in_dim(tokens, here * rows_mine, rows_mine, 0).astype(jnp.float32)
    normed = normalize(tokens.astype(jnp.float32)).astype(jnp.bfloat16)
    order = ((0, 0), (0, 1), (1, 0), (1, 1), (0, 2), (1, 2))
    split = tuple(which < 2 for _, which in order)
    sent = [pieces[layer][which] for layer, which in order]
    whole = dict(zip(order, spread(sent, split, groups, columns)))
    sampler = [
        [whole[layer, which].reshape(columns * block_width, model_width) for which in range(3)]
        for layer in range(2)
    ]
    for layer in range(2):
        flips = sampler[layer]
        gate_flip, up_flip, down_flip = flips
        gate_act = lax.dot_general(normed, gate_flip, contract_last, preferred_element_type=jnp.float32)
        up_act = lax.dot_general(normed, up_flip, contract_last, preferred_element_type=jnp.float32)
        hidden = (jax.nn.silu(gate_act) * up_act).astype(jnp.bfloat16)
        partial = jnp.dot(hidden, down_flip, preferred_element_type=jnp.float32).astype(jnp.bfloat16)
        mixed = lax.psum_scatter(partial, "fs", scatter_dimension=0, tiled=True)
        if layer == 0:
            mixed, first = lax.optimization_barrier((mixed, [emit(flip, 0, None) for flip in flips]))
        mixed = mixed.astype(jnp.float32)
        rounded_state = (residual + 0.5 * out_gain[layer] * normalize(mixed)).astype(jnp.bfloat16)
        if layer == 0:
            residual = rounded_state.astype(jnp.float32)
            normed = normalize(residual).astype(jnp.bfloat16)
            normed, first = lax.optimization_barrier((normed, first))
            normed = lax.all_gather(normed, "fs", axis=0, tiled=True)
            early = emit(sampler[1][0], 1, first[0])
            normed, early = lax.optimization_barrier((normed, early))
            stacked = [early, *first[1:]]
        else:
            stacked[1:] = [emit(flip, 1, held) for flip, held in zip(flips[1:], stacked[1:])]
    return (*stacked, rounded_state)


def solution(mesh):
    in_specs = (
        P(("grp", "tp"), None),
        P(None, "fs", "tp"),
        P(None, "fs", "tp"),
        P(None, "fs", "tp"),
        P(None, "fs"),
        P(),
    )
    out_specs = (
        P("grp", None, "fs"),
        P("grp", None, "fs"),
        P("grp", None, "fs"),
        P(("grp", "tp", "fs"), None),
    )
    return jax.shard_map(body, mesh=mesh, in_specs=in_specs, out_specs=out_specs, check_vma=False)
```

```python
import functools

import jax
import jax.numpy as jnp
from jax import lax
from jax.experimental import pallas as pl
from jax.experimental.pallas import tpu as pltpu
from jax.sharding import PartitionSpec as P

EPS = 1e-06


def normalize(rows):
    return rows * lax.rsqrt(jnp.mean(rows * rows, axis=-1, keepdims=True) + EPS)


def body_plain(tokens, gate_weight, up_weight, down_weight, in_gain, out_gain):
    groups = lax.axis_size("fs")
    rows_all = tokens.shape[0]
    rows_mine = rows_all // groups
    model_width = tokens.shape[1]
    local_rows = gate_weight.shape[1]
    block_width = gate_weight.shape[2] // groups
    residual = lax.dynamic_slice_in_dim(
        tokens, lax.axis_index("fs") * rows_mine, rows_mine, 0
    ).astype(jnp.float32)
    normed = normalize(tokens.astype(jnp.float32)).astype(jnp.bfloat16)
    gates = []
    ups = []
    downs = []
    rounded_state = tokens
    contract_last = (((1,), (1,)), ((), ()))
    for section_idx in range(2):
        scale = in_gain[section_idx][:, None]
        gate_rounded = (scale * gate_weight[section_idx]).astype(jnp.bfloat16)
        up_rounded = (scale * up_weight[section_idx]).astype(jnp.bfloat16)
        down_rounded = down_weight[section_idx].astype(jnp.bfloat16)
        flipped = [
            w.T.reshape(groups, block_width, local_rows)
            for w in (gate_rounded, up_rounded, down_rounded)
        ]
        arrived = (
            lax.all_to_all(flipped[0], "fs", split_axis=0, concat_axis=2, tiled=True),
            lax.all_to_all(flipped[1], "fs", split_axis=0, concat_axis=2, tiled=True),
            lax.all_to_all(flipped[2], "fs", split_axis=0, concat_axis=2, tiled=True),
        )
        thin_rows = [w.reshape(block_width, model_width) for w in arrived]
        sampler_mats = (
            lax.all_gather(thin_rows[0], "tp", axis=0, tiled=True),
            lax.all_gather(thin_rows[1], "tp", axis=0, tiled=True),
            lax.all_gather(thin_rows[2], "tp", axis=0, tiled=True),
        )
        gate_flip, up_flip, down_flip = (sampler_mats[0], sampler_mats[1], sampler_mats[2])
        gates.append(gate_flip.T)
        ups.append(up_flip.T)
        downs.append(down_flip.T)

        def hidden_of(row_block):
            gate_act = lax.dot_general(
                row_block, gate_flip, contract_last, preferred_element_type=jnp.float32
            )
            up_act = lax.dot_general(
                row_block, up_flip, contract_last, preferred_element_type=jnp.float32
            )
            return (jax.nn.silu(gate_act) * up_act).astype(jnp.bfloat16)

        if section_idx == 0:
            hidden = hidden_of(normed)
        else:
            hidden = hidden_of(lax.all_gather(normed, "fs", axis=0, tiled=True))
        mixed = lax.psum_scatter(
            jnp.dot(hidden, down_flip, preferred_element_type=jnp.float32),
            "fs",
            scatter_dimension=0,
            tiled=True,
        )
        rounded_state = (residual + 0.5 * out_gain[section_idx] * normalize(mixed)).astype(
            jnp.bfloat16
        )
        if section_idx == 0:
            residual = rounded_state.astype(jnp.float32)
            normed = normalize(residual).astype(jnp.bfloat16)
    return (jnp.stack(gates), jnp.stack(ups), jnp.stack(downs), rounded_state)


def prep_kernel(blocks, width, part, scaled, where, *refs):
    if scaled:
        gain, weight, out, flip = refs
        rows = weight[0] * gain[0]
    else:
        weight, out, flip = refs
        rows = weight[0]
    flip[...] = rows.astype(jnp.bfloat16).T
    skip = where[0] * part if part < width else 0
    for target in range(blocks):
        start = pl.multiple_of(target * width + skip, 16)
        out[target] = flip[pl.ds(start, part), :]


def prepare(where, weight, gain, layer, blocks, halves):
    _, rows, cols = weight.shape
    width = cols // blocks
    part = width // halves
    step = 256 if rows % 256 == 0 else rows
    in_specs = [pl.BlockSpec((1, step, cols), lambda r, where: (layer, r, 0))]
    args = [weight]
    if gain is not None:
        in_specs.insert(0, pl.BlockSpec((1, step, 1), lambda r, where: (layer, r, 0)))
        args.insert(0, gain)
    return pl.pallas_call(
        functools.partial(prep_kernel, blocks, width, part, gain is not None),
        grid_spec=pltpu.PrefetchScalarGridSpec(
            num_scalar_prefetch=1,
            grid=(rows // step,),
            in_specs=in_specs,
            out_specs=pl.BlockSpec((blocks, part, step), lambda r, where: (0, 0, r)),
            scratch_shapes=[pltpu.VMEM((cols, step), jnp.bfloat16)],
        ),
        out_shape=jax.ShapeDtypeStruct((blocks, part, rows), jnp.bfloat16),
        cost_estimate=pl.CostEstimate(
            flops=rows * cols, bytes_accessed=rows * cols * 5, transcendentals=0
        ),
    )(where, *args)


def spread_kernel(blocks, split, *refs):
    n = len(split)
    sources, full = refs[:n], refs[n : 2 * n]
    own, (own_sem, send_sem, recv_sem) = refs[2 * n : 3 * n], refs[3 * n :]
    y, z, t = lax.axis_index("grp"), lax.axis_index("fs"), lax.axis_index("tp")
    x, c = t // 2, lax.rem(t, 2)
    other_y, other_x, other_c = 1 - y, (1 - x) * 2 + c, x * 2 + (1 - c)
    wide = sources[0].shape[-1]
    partners = [{"fs": lax.rem(z + shift, blocks)} for shift in range(1, blocks)]
    partners += [{"tp": other_x}, {"tp": other_c}, {"grp": other_y}]

    barrier = pltpu.get_barrier_semaphore()
    for partner in partners:
        pl.semaphore_signal(barrier, inc=1, device_id=partner, device_id_type=pl.DeviceIdType.MESH)
    pl.semaphore_wait(barrier, len(partners))

    def columns(source):
        return pl.ds(pl.multiple_of(source * wide, 128), wide)

    def place(m, column, half, source):
        cols = columns(source)
        if not split[m]:
            return full[m].at[column, :, :, cols]
        return full[m].at[column, half, :, cols]

    def rows_of(m, column, half):
        if not split[m]:
            return full[m].at[column]
        return full[m].at[column, half]

    def origin(m, target):
        return sources[m].at[target]

    names = []
    sent = []

    def slot(name):
        if name not in names:
            names.append(name)
        return names.index(name)

    def send(name, source, target, device):
        k = slot(name)
        copy = pltpu.make_async_remote_copy(
            src_ref=source,
            dst_ref=target,
            send_sem=send_sem.at[k],
            recv_sem=recv_sem.at[k],
            device_id=device,
            device_id_type=pl.DeviceIdType.MESH,
        )
        copy.start()
        sent.append(copy)

    def arrived(name, landed, device):
        k = slot(name)
        pltpu.make_async_remote_copy(
            src_ref=landed,
            dst_ref=landed,
            send_sem=send_sem.at[k],
            recv_sem=recv_sem.at[k],
            device_id=device,
            device_id_type=pl.DeviceIdType.MESH,
        ).wait_recv()

    to_x, to_c, to_y = {"tp": other_x}, {"tp": other_c}, {"grp": other_y}
    fetch = []
    for m in range(n):
        for shift in range(1, blocks):
            target = lax.rem(z + shift, blocks)
            send(("z", m, shift), origin(m, target), place(m, t, y, z), {"fs": target})
        mine = origin(m, z)
        send(("x", m, 0), mine, place(m, t, y, z), to_x)
        if split[m]:
            send(("y", m, 0, 0), mine, place(m, t, y, z), to_y)
        copy = pltpu.make_async_copy(mine, own[m], own_sem.at[m])
        copy.start()
        fetch.append(copy)
    kept = []
    for m in range(n):
        fetch[m].wait()
        copy = pltpu.make_async_copy(own[m], place(m, t, y, z), own_sem.at[n + m])
        copy.start()
        kept.append(copy)

    def relay(m, shift):
        source = lax.rem(z + blocks - shift, blocks)
        arrived(("x", m, shift), place(m, other_x, y, source), to_x)
        if split[m]:
            spot = place(m, other_x, y, source)
            send(("y", m, 1, shift), spot, spot, to_y)

    for m in range(n):
        for shift in range(1, blocks):
            source = lax.rem(z + blocks - shift, blocks)
            spot = place(m, t, y, source)
            arrived(("z", m, shift), spot, {"fs": source})
            send(("x", m, shift), spot, spot, to_x)
            if split[m]:
                send(("y", m, 0, shift), spot, spot, to_y)
            relay(m, shift - 1)
        kept[m].wait()
        send(("c", m, 0, 0), rows_of(m, t, y), rows_of(m, t, y), to_c)
        relay(m, blocks - 1)
        send(("c", m, 1, 0), rows_of(m, other_x, y), rows_of(m, other_x, y), to_c)
    for m in range(n):
        if not split[m]:
            continue
        for far, column in ((0, t), (1, other_x)):
            for shift in range(blocks):
                source = lax.rem(z + blocks - shift, blocks)
                arrived(("y", m, far, shift), place(m, column, other_y, source), to_y)
            rows = rows_of(m, column, other_y)
            send(("c", m, far, 1), rows, rows, to_c)
    other_both = (1 - x) * 2 + (1 - c)
    for m in range(n):
        for far, column in ((0, other_c), (1, other_both)):
            arrived(("c", m, far, 0), rows_of(m, column, y), to_c)
            if split[m]:
                arrived(("c", m, far, 1), rows_of(m, column, other_y), to_c)
    for copy in sent:
        copy.wait_send()


def spread(sources, split, blocks, columns):
    n, halves = len(split), 2
    part, rows = sources[0].shape[1:]
    sources = [
        source if alone else source.reshape(blocks, halves, part, rows)
        for source, alone in zip(sources, split)
    ]
    count = sum(4 * blocks + 1 + (2 * blocks + 2) * alone for alone in split)
    shape = (columns, halves, part, rows * blocks)
    moved = n * columns * halves * part * rows * blocks * 2
    whole = pl.BlockSpec(memory_space=pl.ANY)
    return pl.pallas_call(
        functools.partial(spread_kernel, blocks, split),
        in_specs=[whole] * n,
        out_specs=[whole] * n,
        out_shape=[jax.ShapeDtypeStruct(shape, jnp.bfloat16)] * n,
        scratch_shapes=[pltpu.VMEM(source.shape[1:], jnp.bfloat16) for source in sources]
        + [
            pltpu.SemaphoreType.DMA((2 * n,)),
            pltpu.SemaphoreType.DMA((count,)),
            pltpu.SemaphoreType.DMA((count,)),
        ],
        compiler_params=pltpu.CompilerParams(collective_id=0, has_side_effects=True),
        cost_estimate=pl.CostEstimate(flops=0, bytes_accessed=moved * 13, transcendentals=0),
    )(*sources)


def emit_kernel(flip, *refs):
    refs[-1][0] = flip[...].T


def emit(flip, layer, stacked):
    hidden, width = flip.shape
    step = 256
    in_specs = [pl.BlockSpec((hidden, step), lambda r: (0, r))]
    args = [flip]
    aliases = {}
    if stacked is not None:
        in_specs.append(pl.BlockSpec(memory_space=pl.ANY))
        args.append(stacked)
        aliases = {1: 0}
    return pl.pallas_call(
        emit_kernel,
        grid=(width // step,),
        in_specs=in_specs,
        out_specs=pl.BlockSpec((1, step, hidden), lambda r: (layer, r, 0)),
        out_shape=jax.ShapeDtypeStruct((2, width, hidden), jnp.bfloat16),
        input_output_aliases=aliases,
        cost_estimate=pl.CostEstimate(
            flops=0, bytes_accessed=4 * hidden * width, transcendentals=0
        ),
    )(*args)


def body(tokens, gate_weight, up_weight, down_weight, in_gain, out_gain):
    groups = lax.axis_size("fs")
    halves = lax.axis_size("grp")
    block_width = gate_weight.shape[2] // groups
    model_width = tokens.shape[1]
    columns = lax.axis_size("tp")
    odd = block_width % 32 or gate_weight.shape[1] % 128 or gate_weight.shape[2] % 128
    if odd or model_width % 256 or halves != 2 or columns != 4:
        return body_plain(tokens, gate_weight, up_weight, down_weight, in_gain, out_gain)
    rows_mine = tokens.shape[0] // groups
    here = lax.axis_index("fs")
    where = lax.axis_index("grp")[None].astype(jnp.int32)
    gain_column = in_gain[:, :, None]
    contract_last = (((1,), (1,)), ((), ()))
    pieces = [
        [
            prepare(where, gate_weight, gain_column, layer, groups, halves),
            prepare(where, up_weight, gain_column, layer, groups, halves),
            prepare(where, down_weight, None, layer, groups, 1),
        ]
        for layer in range(2)
    ]
    order = ((0, 0), (0, 1), (1, 0), (1, 1), (0, 2), (1, 2))
    split = tuple(which < 2 for _, which in order)
    sent = [pieces[layer][which] for layer, which in order]
    whole = dict(zip(order, spread(sent, split, groups, columns)))
    sampler = [
        [whole[layer, which].reshape(columns * block_width, model_width) for which in range(3)]
        for layer in range(2)
    ]
    def advance(layer, normed, residual):
        gate_flip, up_flip, down_flip = sampler[layer]
        gate_act = lax.dot_general(normed, gate_flip, contract_last, preferred_element_type=jnp.float32)
        up_act = lax.dot_general(normed, up_flip, contract_last, preferred_element_type=jnp.float32)
        hidden = (jax.nn.silu(gate_act) * up_act).astype(jnp.bfloat16)
        partial = jnp.dot(hidden, down_flip, preferred_element_type=jnp.float32).astype(jnp.bfloat16)
        mixed = lax.psum_scatter(partial, "fs", scatter_dimension=0, tiled=True).astype(jnp.float32)
        return (residual + 0.5 * out_gain[layer] * normalize(mixed)).astype(jnp.bfloat16)

    folded = tokens.reshape(groups, 2, rows_mine // 2, model_width)
    states = []
    for side in range(2):
        rows = folded[:, side].reshape(groups * rows_mine // 2, model_width)
        kept = lax.dynamic_index_in_dim(folded[:, side], here, 0, keepdims=False)
        normed = normalize(rows.astype(jnp.float32)).astype(jnp.bfloat16)
        states.append(advance(0, normed, kept.astype(jnp.float32)))
    stacked = [emit(flip, 0, None) for flip in sampler[0]]
    states[1], stacked[:2] = lax.optimization_barrier((states[1], stacked[:2]))
    ends = []
    for state in states:
        residual = state.astype(jnp.float32)
        normed = lax.all_gather(normalize(residual).astype(jnp.bfloat16), "fs", axis=0, tiled=True)
        ends.append(advance(1, normed, residual))
    stacked = [emit(flip, 1, held) for flip, held in zip(sampler[1], stacked)]
    rounded_state = jnp.concatenate(ends)
    return (*stacked, rounded_state)


def solution(mesh):
    in_specs = (
        P(("grp", "tp"), None),
        P(None, "fs", "tp"),
        P(None, "fs", "tp"),
        P(None, "fs", "tp"),
        P(None, "fs"),
        P(),
    )
    out_specs = (
        P("grp", None, "fs"),
        P("grp", None, "fs"),
        P("grp", None, "fs"),
        P(("grp", "tp", "fs"), None),
    )
    return jax.shard_map(body, mesh=mesh, in_specs=in_specs, out_specs=out_specs, check_vma=False)
```
